256 devices in a mesh: ep: 128 (over z, y, x), tp: 2 (over core).
Axes of the slice: x: 4, y: 4, z: 8, core: 2. Of those that a mesh axis runs over, the one named last changes fastest.
Arguments:
- tokens: bfloat16 [2048, 2048], P('ep'), may hold values from -6 to 6
- recurrent_state: float32 [2048, 4, 128, 256], P('ep', 'tp'), may hold values from -6 to 6
- query_weight: bfloat16 [2048, 512], P(None, 'tp'), may hold values from -0.125 to 0.125
- key_weight: bfloat16 [2048, 512], P(None, 'tp'), may hold values from -0.125 to 0.125
- decay_weight: bfloat16 [2048, 512], P(None, 'tp'), may hold values from -0.5 to 0.5
- value_weight: bfloat16 [2048, 1024], P(None, 'tp'), may hold values from -0.125 to 0.125
- gate_weight: bfloat16 [2048, 1024], P(None, 'tp'), may hold values from -0.125 to 0.125
- head_gain: float32 [256], replicated, may hold values from 0.1 to 1.9
- output_weight: bfloat16 [1024, 2048], P('tp'), may hold values from -0.375 to 0.375
- norm_gain: float32 [2, 2048], replicated, may hold values from 0.1 to 1.9
- norm_bias: float32 [2, 2048], replicated, may hold values from -1.8 to 1.8
- group_router: bfloat16 [2048, 4], replicated, may hold values from -0.125 to 0.125
- router_weight: bfloat16 [2048, 256], replicated, may hold values from -0.125 to 0.125
- routes: int32 [2048, 2], P('ep'), may hold values from 0 to 255, as said below
- expert_gate: bfloat16 [256, 2048, 256], P(('ep', 'tp')), may hold values from -0.125 to 0.125
- expert_up: bfloat16 [256, 2048, 256], P(('ep', 'tp')), may hold values from -0.125 to 0.125
- expert_down: bfloat16 [256, 256, 2048], P(('ep', 'tp')), may hold values from -1.5 to 1.5
Outputs:
- new_tokens: bfloat16 [2048, 2048], P('ep', 'tp')
- new_state: float32 [2048, 4, 128, 256], P('ep', 'tp')
The draws below stay inside these ranges and needn't reach their ends.
Inputs may be any that keep to these rules, and one draw needn't show every extreme that they name: `routes`: each row names two different experts of one group (group g holds the experts g * 64 to g * 64 + 63). In the rows of one device each group is named by the same number of rows and no expert by more than 2 rows; some expert is named by exactly 2 rows of every device.
All inputs are finite; a program needn't handle non-finite values.
Results may differ from the reference program's by a relative error of at most 0.01.
Values may be sent and summed in bfloat16 or wider, within the bound.
A program may use at most 128 MiB of HBM per device.

```python
import jax
import jax.numpy as jnp
from jax import lax

D = 2048
HEADS = 4
DK = 128
DV = 256
EXPERT_FF = 256
GROUPS = 4
TOPK = 2
SEQ_DEV = 16
KW = 512
VW = 1024
EXPERTS = 256
EPG = 64
BATCH = 2048
CAP = 2
N_EP = 128
N_TP = 2


def draw_routes(key, part):
    per_group = EXPERTS // GROUPS
    block_keys = jax.random.split(jax.random.fold_in(key, 11), N_EP)

    def permute(subkey):
        return jax.random.permutation(subkey, SEQ_DEV)
    rank_order = jax.vmap(permute)(block_keys).astype(jnp.int32)
    group_id = rank_order % GROUPS
    within_group = rank_order // GROUPS
    offsets = jax.random.randint(jax.random.fold_in(key, 12), (N_EP, GROUPS), 0, per_group).astype(jnp.int32)
    offsets = offsets.at[0, 0].set(0).at[0, GROUPS - 1].set(per_group - 1)
    extra_gap = jax.random.randint(jax.random.fold_in(key, 14), (N_EP, GROUPS), 0, 2).astype(jnp.int32)
    row_offset = jnp.take_along_axis(offsets, group_id, axis=1)
    row_gap = jnp.take_along_axis(extra_gap, group_id, axis=1)
    first_pick = group_id * per_group + (within_group + row_offset) % per_group
    second_pick = group_id * per_group + (within_group + row_offset + 1 + row_gap) % per_group
    flip_bits = jax.random.randint(jax.random.fold_in(key, 13), (N_EP, SEQ_DEV), 0, 2)
    lead_pick = jnp.where(flip_bits == 1, second_pick, first_pick)
    trail_pick = jnp.where(flip_bits == 1, first_pick, second_pick)
    return jnp.stack([lead_pick, trail_pick], axis=-1).reshape(BATCH, 2).astype(jnp.int32)


def level_of(own_key, extent, shards, smallest, largest):
    gain = 1.0
    for position, shards_of in shards:
        steps = jax.random.uniform(jax.random.fold_in(jax.random.fold_in(own_key, 6), position), (shards_of,), jnp.float32, smallest / len(shards), largest / len(shards))
        gain = gain * jnp.repeat(jnp.exp(steps), extent[position] // shards_of).reshape((-1,) + (1,) * (len(extent) - 1 - position))
    return gain


def centred(own_key, extent, width, bound, cuts=(), kind=jnp.bfloat16):
    array = width * jax.random.normal(own_key, extent, jnp.float32)
    if cuts:
        array = array * level_of(own_key, extent, cuts, -0.22, 0.18)
    return jnp.clip(array, -bound, bound).astype(kind)


def setup_inputs(seed: int = 0) -> dict:
    key_list = jax.random.split(jax.random.key(seed), 18)
    return {
        "tokens": centred(key_list[0], (BATCH, D), 1.0, 6.0, ((0, 128),)),
        "recurrent_state": centred(key_list[1], (BATCH, HEADS, DK, DV), 1.0, 6.0, ((0, 128), (1, 2)), jnp.float32),
        "query_weight": centred(key_list[2], (D, KW), D ** -0.5, 0.125, ((1, 2),)),
        "key_weight": centred(key_list[3], (D, KW), D ** -0.5, 0.125, ((1, 2),)),
        "decay_weight": centred(key_list[4], (D, KW), (D // 16) ** -0.5, 0.5, ((1, 2),)),
        "value_weight": centred(key_list[5], (D, VW), D ** -0.5, 0.125, ((1, 2),)),
        "gate_weight": centred(key_list[6], (D, VW), D ** -0.5, 0.125, ((1, 2),)),
        "head_gain": jnp.clip(1.0 + 0.18 * jax.random.normal(key_list[7], (DV,), jnp.float32), 0.1, 1.9),
        "output_weight": centred(key_list[8], (VW, D), (VW // 4) ** -0.5, 0.375, ((0, 2),)),
        "norm_gain": jnp.clip(1.0 + 0.18 * jax.random.normal(key_list[9], (2, D), jnp.float32), 0.1, 1.9),
        "norm_bias": centred(key_list[10], (2, D), 0.3, 1.8, (), jnp.float32),
        "group_router": centred(key_list[11], (D, GROUPS), D ** -0.5, 0.125),
        "router_weight": centred(key_list[12], (D, EXPERTS), D ** -0.5, 0.125),
        "routes": draw_routes(jax.random.fold_in(key_list[17], 71), 0),
        "expert_gate": centred(key_list[14], (EXPERTS, D, EXPERT_FF), D ** -0.5, 0.125, ((0, 256),)),
        "expert_up": centred(key_list[15], (EXPERTS, D, EXPERT_FF), D ** -0.5, 0.125, ((0, 256),)),
        "expert_down": centred(key_list[16], (EXPERTS, EXPERT_FF, D), (EXPERT_FF // 16) ** -0.5, 1.5, ((0, 256),)),
    }


alpha_res = 2.0 ** 0.5
eps_norm = 1e-05

def layer_normed(inputs, gain_row, bias_row):
    centered = inputs - lax.optimization_barrier(jnp.mean(inputs, axis=-1, keepdims=True))
    spread = lax.optimization_barrier(jnp.mean(centered * centered, axis=-1, keepdims=True))
    return centered * lax.rsqrt(spread + eps_norm) * gain_row + bias_row

def rounded_back(values_in):
    return lax.optimization_barrier(values_in.astype(jnp.bfloat16)).astype(jnp.float32)

def reference(tokens, recurrent_state, query_weight, key_weight, decay_weight, value_weight, gate_weight, head_gain, output_weight, norm_gain, norm_bias, group_router, router_weight, routes, expert_gate, expert_up, expert_down):

    def project(weight):
        return jnp.dot(tokens, weight, preferred_element_type=jnp.float32)
    queries = project(query_weight).reshape(BATCH, HEADS, DK) * DK ** (-0.5)
    key_rows = project(key_weight).reshape(BATCH, HEADS, DK)
    value_rows = project(value_weight).reshape(BATCH, HEADS, DV)
    gate_rows = project(gate_weight)
    log_decay = (jax.nn.log_sigmoid(project(decay_weight)) / 16.0).reshape(BATCH, HEADS, DK)
    new_state = jnp.exp(log_decay)[..., None] * recurrent_state + key_rows[..., None] * value_rows[:, :, None, :]
    readout = lax.optimization_barrier(jnp.sum(queries[..., None] * new_state, axis=2))
    norm_scale = lax.rsqrt(lax.optimization_barrier(jnp.mean(readout * readout, axis=-1, keepdims=True)) + eps_norm)
    gated = ((readout * norm_scale * head_gain).reshape(BATCH, VW) * jax.nn.silu(gate_rows)).astype(jnp.bfloat16)
    group_cols = VW // N_TP
    mixed_sum = jnp.zeros((BATCH, D), jnp.float32)
    for part_index in range(N_TP):
        product_part = jnp.dot(gated[:, part_index * group_cols:(part_index + 1) * group_cols], output_weight[part_index * group_cols:(part_index + 1) * group_cols], preferred_element_type=jnp.float32)
        mixed_sum = mixed_sum + rounded_back(product_part)
    hidden = layer_normed(alpha_res * tokens.astype(jnp.float32) + mixed_sum, norm_gain[0], norm_bias[0]).astype(jnp.bfloat16)
    group_logit = jnp.dot(hidden, group_router, preferred_element_type=jnp.float32)
    expert_logit = jnp.dot(hidden, router_weight, preferred_element_type=jnp.float32)
    chosen_group = routes[:, 0] // EPG
    group_hit = chosen_group[:, None] == jnp.arange(GROUPS, dtype=jnp.int32)[None, :]
    own_logit = lax.optimization_barrier(jnp.sum(jnp.where(group_hit, group_logit, 0.0), axis=1, keepdims=True))
    group_share = 1.0 / lax.optimization_barrier(jnp.sum(jnp.exp(group_logit - own_logit), axis=1))
    expert_hit = routes[:, :, None] == jnp.arange(EXPERTS, dtype=jnp.int32)[None, None, :]
    picked = lax.optimization_barrier(jnp.sum(jnp.where(expert_hit, expert_logit[:, None, :], 0.0), axis=2))
    route_weight = group_share[:, None] * jax.nn.sigmoid(picked - picked[:, ::-1])
    flat_routes = routes.reshape(BATCH * TOPK)
    row_limit = N_EP * CAP

    def serve_expert(expert_index):
        hit_index = jnp.nonzero(flat_routes == expert_index, size=row_limit, fill_value=BATCH * TOPK)[0].astype(jnp.int32)
        rows_in = hidden[jnp.minimum(hit_index, BATCH * TOPK - 1) // TOPK]
        gate_part = jnp.dot(rows_in, expert_gate[expert_index], preferred_element_type=jnp.float32)
        up_part = jnp.dot(rows_in, expert_up[expert_index], preferred_element_type=jnp.float32)
        activation = (jax.nn.silu(gate_part) * up_part).astype(jnp.bfloat16)
        combined = jnp.dot(activation, expert_down[expert_index], preferred_element_type=jnp.float32)
        return (hit_index, combined.astype(jnp.bfloat16))
    all_index, all_out = lax.map(serve_expert, jnp.arange(EXPERTS, dtype=jnp.int32))
    expert_out = jnp.zeros((BATCH * TOPK, D), jnp.bfloat16).at[all_index.reshape(-1)].set(all_out.reshape(-1, D), mode='drop')
    routed_sum = lax.optimization_barrier(jnp.sum(route_weight[..., None] * expert_out.reshape(BATCH, TOPK, D).astype(jnp.float32), axis=1))
    new_tokens = layer_normed(alpha_res * hidden.astype(jnp.float32) + routed_sum, norm_gain[1], norm_bias[1]).astype(jnp.bfloat16)
    return (new_tokens, new_state)
```

```python
import functools

import jax
import jax.numpy as jnp
from jax import lax
from jax.experimental import pallas as pl
from jax.experimental.pallas import tpu as pltpu
from jax.sharding import PartitionSpec as P

MESH = pl.DeviceIdType.MESH
BF16 = jnp.bfloat16
F32 = jnp.float32
ROOT2 = 2.0**0.5
EPS = 1e-05

NX, NY, NZ = 4, 4, 8
ROWS = 16
WIDTH = 2048
HALF = 1024
CARRY = HALF + 128
FOLD = 256
SLAB = FOLD + 128
OFF = (0, 1, -1, 2)
OFFZ = (0, 1, -1, 2, -2, 3, -3, 4)
VIA_PLUS = (0, 3)
VIA_MINUS = (1, 2)
NCOPY = 128


def iota(shape, dim):
    return lax.broadcasted_iota(jnp.int32, shape, dim)


def where_bf16(mask):
    return jnp.where(mask, 1.0, 0.0).astype(BF16)


def dotf(a, b):
    return jnp.dot(a, b, preferred_element_type=F32)


def moe_kernel(
    gated_ref,
    tokens_ref,
    gain_ref,
    bias_ref,
    group_ref,
    routes_ref,
    wo_hbm,
    router_hbm,
    gate_hbm,
    up_hbm,
    down_hbm,
    out_ref,
    wo_v,
    router_v,
    gate_v,
    up_v,
    down_v,
    xs,
    xr,
    hid,
    zs,
    zr,
    own,
    part,
    ps,
    pr,
    red,
    fwd_in,
    top_in,
    low_in,
    low_out,
    fin,
    zback,
    zret,
    st_s,
    st_r,
    local_sem,
    send_sem,
    recv_sem,
):
    ep = lax.axis_index("ep")
    core = lax.axis_index("tp")
    x = lax.rem(ep, NX)
    y = lax.rem(ep // NX, NY)
    z = ep // (NX * NY)

    def device(dx=0, dy=0, dz=0, flip=False):
        ex = lax.rem(x + (dx + NX), NX)
        ey = lax.rem(y + (dy + NY), NY)
        ez = lax.rem(z + (dz + NZ), NZ)
        return {"ep": (ez * NY + ey) * NX + ex, "tp": (1 - core) if flip else core}

    def along(first, step):
        return device(dx=step) if first else device(dy=step)

    pair = device(flip=True)
    peers = [pair]
    peers += [device(dz=d) for d in OFFZ[1:]]
    peers += [device(dx=d) for d in OFF[1:]]
    peers += [device(dy=d) for d in OFF[1:]]
    barrier = pltpu.get_barrier_semaphore()
    for peer in peers:
        pl.semaphore_signal(barrier, inc=1, device_id=peer, device_id_type=MESH)

    loads = []
    for n, (src, dst) in enumerate(
        (
            (wo_hbm, wo_v),
            (router_hbm, router_v),
            (gate_hbm.at[0], gate_v),
            (up_hbm.at[0], up_v),
            (down_hbm.at[0], down_v),
        )
    ):
        load = pltpu.make_async_copy(src, dst, local_sem.at[n])
        load.start()
        loads.append(load)

    made = []

    def send(src, dst, to):
        n = len(made)
        copy = pltpu.make_async_remote_copy(
            src_ref=src,
            dst_ref=dst,
            send_sem=send_sem.at[n],
            recv_sem=recv_sem.at[n],
            device_id=to,
            device_id_type=MESH,
        )
        copy.start()
        made.append(copy)
        return copy

    loads[0].wait()
    partial_bf = dotf(gated_ref[...], wo_v[...]).astype(BF16)
    xs[...] = partial_bf
    pl.semaphore_wait(barrier, len(peers))
    exchange = send(xs, xr, pair)
    mixed = ROOT2 * tokens_ref[...].astype(F32) + partial_bf.astype(F32)

    routes = routes_ref[...]
    first_route, second_route = routes[:, 0:1], routes[:, 1:2]
    group_col = lax.shift_right_logical(first_route, 6)
    lanes = iota((ROWS, 128), 1)
    onehot_group = where_bf16(lanes == group_col)
    lower = where_bf16(iota((ROWS, ROWS), 0) > iota((ROWS, ROWS), 1))
    earlier = dotf(lower, onehot_group)
    rank_col = jnp.sum(jnp.where(lanes == group_col, earlier, 0.0), axis=1, keepdims=True)
    place_col = group_col.astype(F32) * 4.0 + rank_col
    diagonal = jnp.where(iota((ROWS, ROWS), 0) == iota((ROWS, ROWS), 1), place_col, 0.0)
    place_row = dotf(jnp.ones((64, ROWS), BF16), diagonal.astype(BF16))
    slab_row = iota((64, ROWS), 0)
    wanted = ((slab_row >> 4) * 4 + (slab_row & 3)).astype(F32)
    quarter = (slab_row >> 2) & 3
    match = place_row == wanted

    exchange.wait_recv()
    mixed = mixed + xr[...].astype(F32)
    mean = jnp.mean(mixed, axis=-1, keepdims=True)
    centered = mixed - mean
    spread = jnp.mean(centered * centered, axis=-1, keepdims=True)
    hidden = (
        centered * lax.rsqrt(spread + EPS) * gain_ref[0:1, :] + bias_ref[0:1, :]
    ).astype(BF16)
    hid[...] = hidden

    loads[1].wait()
    expert_logit = dotf(hidden, router_v[...])
    hidden_f = hidden.astype(F32)
    group_logit = [
        jnp.sum(hidden_f * group_ref[g : g + 1, :].astype(F32), axis=1, keepdims=True)
        for g in range(4)
    ]
    own_logit = jnp.zeros_like(group_logit[0])
    for g in range(4):
        own_logit = own_logit + jnp.where(group_col == g, group_logit[g], 0.0)
    share_sum = jnp.zeros_like(own_logit)
    for g in range(4):
        share_sum = share_sum + jnp.exp(group_logit[g] - own_logit)
    share = 1.0 / share_sum
    wide = iota((ROWS, 256), 1)
    picked0 = jnp.sum(jnp.where(wide == first_route, expert_logit, 0.0), axis=1, keepdims=True)
    picked1 = jnp.sum(jnp.where(wide == second_route, expert_logit, 0.0), axis=1, keepdims=True)
    weight0 = share * jax.nn.sigmoid(picked0 - picked1)
    weight1 = share * jax.nn.sigmoid(picked1 - picked0)
    meta = (
        jnp.where(lanes == (first_route & 63), weight0, 0.0)
        + jnp.where(lanes == (second_route & 63), weight1, 0.0)
    ).astype(BF16)

    my_cols = pl.multiple_of(core * HALF, HALF)
    other_cols = pl.multiple_of((1 - core) * HALF, HALF)
    slabs = jnp.zeros((64, FOLD), F32)
    for q in range(4):
        pick = where_bf16(match & (quarter == q))
        slabs = slabs + dotf(pick, hid[:, pl.ds(pl.multiple_of(my_cols + q * FOLD, FOLD), FOLD)])
    slab_meta = dotf(where_bf16(match & (quarter == 0)), meta)
    zs[:, :, 0:FOLD] = slabs.astype(BF16).reshape(4, 16, FOLD)
    zs[:, :, FOLD:SLAB] = slab_meta.astype(BF16).reshape(4, 16, 128)
    z_sends = [None]
    for k in range(1, NZ):
        to_z = lax.rem(z + (OFFZ[k] + NZ), NZ)
        z_sends.append(send(zs.at[to_z // 2], zr.at[k], device(dz=OFFZ[k])))
    zr[0] = zs[z // 2]

    out_i = iota((64, 64), 0)
    in_i = iota((64, 64), 1)
    unfold = where_bf16(
        in_i == ((out_i >> 2) & 3) * 16 + (out_i >> 4) * 4 + (out_i & 3)
    )

    def slot(i, h, j):
        return i * 8 + h * 4 + j

    arrive = {}

    def p1_sends(h):
        for j in (3, 1, 2):
            arrive[0, h, j] = send(
                own.at[slot(0, h, 0)], own.at[slot(0, h, j)], along(h == 0, OFF[j])
            )

    def p2_sends(h, j):
        for i in (1, 2):
            arrive[i, h, j] = send(
                own.at[slot(0, h, j)], own.at[slot(i, h, j)], along(h == 1, OFF[i])
            )

    def forward(h, j):
        i = 1 if j in VIA_PLUS else 2
        arrive[i, h, j].wait_recv()
        arrive[3, h, j] = send(
            own.at[slot(i, h, j)], own.at[slot(3, h, j)], along(h == 1, OFF[i])
        )

    def to_pair(first, count):
        return send(
            own.at[pl.ds(first, count), :, pl.ds(0, HALF)],
            part.at[pl.ds(first, count)],
            pair,
        )

    for h in range(2):
        for k in range(4 * h, 4 * h + 4):
            if k:
                z_sends[k].wait_recv()
        block = dotf(unfold, zr[4 * h : 4 * h + 4].reshape(64, SLAB)).astype(BF16)
        for q in range(4):
            own[slot(0, h, 0), :, q * FOLD : (q + 1) * FOLD] = block[
                q * 16 : (q + 1) * 16, 0:FOLD
            ]
        own[slot(0, h, 0), :, HALF:CARRY] = block[0:16, FOLD:SLAB]
        p1_sends(h)
        p2_sends(h, 0)

    half_copies = {}
    for h in range(2):
        for j in (1, 2, 3):
            arrive[0, h, j].wait_recv()
            p2_sends(h, j)
        half_copies[0, h] = to_pair(slot(0, h, 0), 4)
    for j in (0, 1, 2, 3):
        for h in range(2):
            forward(h, j)

    my_expert = lax.rem(ep, 32) * 2 + core

    for load in loads[2:]:
        load.wait()

    def experts(i, count):
        rows = count * 128
        first = i * 8
        mine = own[first : first + count * 8, :, 0:HALF].reshape(rows, HALF)
        theirs = part[first : first + count * 8].reshape(rows, HALF)
        marks = own[first : first + count * 8, :, HALF:CARRY].reshape(rows, 128).astype(F32)
        weight = jnp.sum(
            jnp.where(iota((rows, 128), 1) == my_expert, marks, 0.0), axis=1, keepdims=True
        )
        my_rows, other_rows = pl.ds(my_cols, HALF), pl.ds(other_cols, HALF)
        gate = dotf(mine, gate_v[my_rows, :]) + dotf(theirs, gate_v[other_rows, :])
        up = dotf(mine, up_v[my_rows, :]) + dotf(theirs, up_v[other_rows, :])
        act = (jax.nn.silu(gate) * up).astype(BF16)
        away = dotf(act, down_v[:, pl.ds(other_cols, HALF)]) * weight
        ps[first : first + count * 8] = away.astype(BF16).reshape(count * 8, 16, HALF)
        copy = send(
            ps.at[pl.ds(first, count * 8)], pr.at[pl.ds(first, count * 8)], pair
        )
        here = dotf(act, down_v[:, pl.ds(my_cols, HALF)]) * weight
        red[first : first + count * 8] = here.astype(BF16).reshape(count * 8, 16, HALF)
        return copy

    def add_pair(copy, i, count):
        copy.wait_recv()
        span = slice(i * 8, (i + count) * 8)
        red[span] = (red[span].astype(F32) + pr[span].astype(F32)).astype(BF16)

    for h in range(2):
        half_copies[0, h].wait_recv()
    result0 = experts(0, 1)

    for i in (1, 2):
        for h in range(2):
            for j in range(4):
                if (i == 1) != (j in VIA_PLUS):
                    arrive[i, h, j].wait_recv()
    middle = to_pair(8, 16)
    add_pair(result0, 0, 1)
    middle.wait_recv()
    result1 = experts(1, 2)
    for h in range(2):
        for j in range(4):
            arrive[3, h, j].wait_recv()
    last = to_pair(24, 8)
    add_pair(result1, 1, 2)

    top = {}

    def top_send(i, h, j):
        top[i, h, j] = send(
            red.at[slot(i, h, j)],
            top_in.at[(i - 1) * 8 + h * 4 + j],
            along(h == 1, -OFF[i]),
        )

    for h in range(2):
        for j in VIA_MINUS:
            top_send(1, h, j)
        for j in VIA_PLUS:
            top_send(2, h, j)
    last.wait_recv()
    result2 = experts(3, 1)
    add_pair(result2, 3, 1)
    back = {}
    for h in range(2):
        for j in range(4):
            i = 1 if j in VIA_PLUS else 2
            back[h, j] = send(
                red.at[slot(3, h, j)], fwd_in.at[h * 4 + j], along(h == 1, -OFF[i])
            )
    for h in range(2):
        for j in range(4):
            i = 1 if j in VIA_PLUS else 2
            back[h, j].wait_recv()
            s = slot(i, h, j)
            red[s] = (red[s].astype(F32) + fwd_in[h * 4 + j].astype(F32)).astype(BF16)
            top_send(i, h, j)
    low = {}
    for j in (3, 1, 2, 0):
        for h in range(2):
            total = red[slot(0, h, j)].astype(F32)
            for i in (1, 2):
                top[i, h, j].wait_recv()
                total = total + top_in[(i - 1) * 8 + h * 4 + j].astype(F32)
            if j:
                low_out[h * 4 + j] = total.astype(BF16)
                low[h, j] = send(
                    low_out.at[h * 4 + j], low_in.at[h * 4 + j], along(h == 0, -OFF[j])
                )
            else:
                fin[h] = total

    fold_i = iota((64, 16), 0)
    fold_o = iota((64, 16), 1)
    fold_match = fold_o == (fold_i >> 4) * 4 + (fold_i & 3)
    fold_quarter = (fold_i >> 2) & 3
    z_back = [None]
    for h in range(2):
        total = fin[h]
        for j in (1, 2, 3):
            low[h, j].wait_recv()
            total = total + low_in[h * 4 + j].astype(F32)
        total = total.astype(BF16)
        folded = jnp.zeros((64, FOLD), F32)
        for q in range(4):
            folded = folded + dotf(
                where_bf16(fold_match & (fold_quarter == q)),
                total[:, q * FOLD : (q + 1) * FOLD],
            )
        zback[4 * h : 4 * h + 4] = folded.astype(BF16).reshape(4, 16, FOLD)
        for k in range(4 * h, 4 * h + 4):
            if k:
                z_back.append(send(zback.at[k], zret.at[k], device(dz=-OFFZ[k])))
    zret[0] = zback[0]

    take_o = iota((64, 128), 0)
    take_i = iota((64, 128), 1)
    slab_k = take_i >> 4
    away_k = (slab_k + 1) >> 1
    signed = jnp.where((slab_k & 1) == 1, away_k, -away_k)
    plane = (z + signed + NZ) & (NZ - 1)
    expected = ((plane >> 1) * 4 + (take_i & 3)).astype(F32)
    place_tall = jnp.concatenate([place_col] * 4, axis=0)
    take = where_bf16(
        (expected == place_tall) & ((take_o >> 4) == ((take_i >> 2) & 3))
    )
    for k in range(1, NZ):
        z_back[k].wait_recv()
    routed = dotf(take, zret[...].reshape(128, FOLD))
    routed = jnp.concatenate([routed[q * 16 : (q + 1) * 16] for q in range(4)], axis=1)
    blended = ROOT2 * hid[:, pl.ds(my_cols, HALF)].astype(F32) + routed
    row_sum = jnp.sum(blended, axis=1, keepdims=True)
    row_sq = jnp.sum(blended * blended, axis=1, keepdims=True)
    st_s[...] = jnp.where(lanes == 0, row_sum, row_sq)
    stats = send(st_s, st_r, pair)
    stats.wait_recv()
    row_mean = (row_sum + st_r[:, 0:1]) / WIDTH
    spread = (row_sq + st_r[:, 1:2]) / WIDTH - row_mean * row_mean
    out_ref[...] = (
        (blended - row_mean)
        * lax.rsqrt(spread + EPS)
        * gain_ref[1:2, pl.ds(my_cols, HALF)]
        + bias_ref[1:2, pl.ds(my_cols, HALF)]
    ).astype(BF16)
    for copy in made:
        copy.wait_send()


def moe(gated, tokens, gain, bias, group_rows, routes, wo, router, gate, up, down):
    vmem = pl.BlockSpec(memory_space=pltpu.VMEM)
    anywhere = pl.BlockSpec(memory_space=pl.ANY)
    return pl.pallas_call(
        moe_kernel,
        out_shape=jax.ShapeDtypeStruct((ROWS, HALF), BF16),
        in_specs=[vmem] * 6 + [anywhere] * 5,
        out_specs=vmem,
        scratch_shapes=[
            pltpu.VMEM((512, WIDTH), BF16),
            pltpu.VMEM((WIDTH, 256), BF16),
            pltpu.VMEM((WIDTH, 256), BF16),
            pltpu.VMEM((WIDTH, 256), BF16),
            pltpu.VMEM((256, WIDTH), BF16),
            pltpu.VMEM((ROWS, WIDTH), BF16),
            pltpu.VMEM((ROWS, WIDTH), BF16),
            pltpu.VMEM((ROWS, WIDTH), BF16),
            pltpu.VMEM((4, 16, SLAB), BF16),
            pltpu.VMEM((8, 16, SLAB), BF16),
            pltpu.VMEM((32, 16, CARRY), BF16),
            pltpu.VMEM((32, 16, HALF), BF16),
            pltpu.VMEM((32, 16, HALF), BF16),
            pltpu.VMEM((32, 16, HALF), BF16),
            pltpu.VMEM((32, 16, HALF), BF16),
            pltpu.VMEM((8, 16, HALF), BF16),
            pltpu.VMEM((16, 16, HALF), BF16),
            pltpu.VMEM((8, 16, HALF), BF16),
            pltpu.VMEM((8, 16, HALF), BF16),
            pltpu.VMEM((2, 16, HALF), F32),
            pltpu.VMEM((8, 16, FOLD), BF16),
            pltpu.VMEM((8, 16, FOLD), BF16),
            pltpu.VMEM((ROWS, 128), F32),
            pltpu.VMEM((ROWS, 128), F32),
            pltpu.SemaphoreType.DMA((5,)),
            pltpu.SemaphoreType.DMA((NCOPY,)),
            pltpu.SemaphoreType.DMA((NCOPY,)),
        ],
        compiler_params=pltpu.CompilerParams(
            collective_id=0, has_side_effects=True, vmem_limit_bytes=40 * 1024 * 1024
        ),
        name="route_and_experts",
    )(gated, tokens, gain, bias, group_rows, routes, wo, router, gate, up, down)


def on_device(
    tokens,
    recurrent_state,
    query_weight,
    key_weight,
    decay_weight,
    value_weight,
    gate_weight,
    head_gain,
    output_weight,
    norm_gain,
    norm_bias,
    group_router,
    router_weight,
    routes,
    expert_gate,
    expert_up,
    expert_down,
):
    row_count, model_width = tokens.shape
    heads_here = recurrent_state.shape[1]
    key_dim = recurrent_state.shape[2]
    value_dim = recurrent_state.shape[3]

    def project(weight):
        return jnp.dot(tokens, weight, preferred_element_type=jnp.float32)

    queries = project(query_weight).reshape(row_count, heads_here, key_dim) * key_dim ** (-0.5)
    key_rows = project(key_weight).reshape(row_count, heads_here, key_dim)
    value_rows = project(value_weight).reshape(row_count, heads_here, value_dim)
    gate_rows = project(gate_weight)
    decay_rate = jnp.exp(jax.nn.log_sigmoid(project(decay_weight)) / 16.0).reshape(
        row_count, heads_here, key_dim
    )
    new_state = (
        decay_rate[..., None] * recurrent_state + key_rows[..., None] * value_rows[:, :, None, :]
    )
    readout = jnp.sum(queries[..., None] * new_state, axis=2)
    norm_scale = lax.rsqrt(jnp.mean(readout * readout, axis=-1, keepdims=True) + EPS)
    gated_rows = (
        (readout * norm_scale * head_gain).reshape(row_count, heads_here * value_dim)
        * jax.nn.silu(gate_rows)
    ).astype(jnp.bfloat16)
    new_tokens = moe(
        gated_rows,
        tokens,
        norm_gain,
        norm_bias,
        group_router.T,
        routes,
        output_weight,
        router_weight,
        expert_gate,
        expert_up,
        expert_down,
    )
    return (new_tokens, new_state)


def solution(mesh):
    in_specs = (
        P("ep", None),
        P("ep", "tp", None, None),
        P(None, "tp"),
        P(None, "tp"),
        P(None, "tp"),
        P(None, "tp"),
        P(None, "tp"),
        P(),
        P("tp", None),
        P(),
        P(),
        P(),
        P(),
        P("ep", None),
        P(("ep", "tp"), None, None),
        P(("ep", "tp"), None, None),
        P(("ep", "tp"), None, None),
    )
    out_specs = (P("ep", "tp"), P("ep", "tp", None, None))
    return jax.shard_map(
        on_device, mesh=mesh, in_specs=in_specs, out_specs=out_specs, check_vma=False
    )
```

```python
import functools

import jax
import jax.numpy as jnp
from jax import lax
from jax.experimental import pallas as pl
from jax.experimental.pallas import tpu as pltpu
from jax.sharding import PartitionSpec as P

MESH = pl.DeviceIdType.MESH
BF16 = jnp.bfloat16
F32 = jnp.float32
ROOT2 = 2.0**0.5
EPS = 1e-05

NX, NY, NZ = 4, 4, 8
ROWS = 16
WIDTH = 2048
HALF = 1024
CARRY = HALF + 128
FOLD = 256
SLAB = FOLD + 128
OFF = (0, 1, -1, 2)
OFFZ = (0, 1, -1, 2, -2, 3, -3, 4)
VIA_PLUS = (0, 3)
VIA_MINUS = (1, 2)
NCOPY = 128


def iota(shape, dim):
    return lax.broadcasted_iota(jnp.int32, shape, dim)


def where_bf16(mask):
    return jnp.where(mask, 1.0, 0.0).astype(BF16)


def dotf(a, b):
    return jnp.dot(a, b, preferred_element_type=F32)


def moe_kernel(
    gated_ref,
    tokens_ref,
    gain_ref,
    bias_ref,
    group_ref,
    routes_ref,
    wo_hbm,
    router_hbm,
    gate_hbm,
    up_hbm,
    down_hbm,
    out_ref,
    wo_v,
    router_v,
    gate_v,
    up_v,
    down_v,
    xs,
    xr,
    hid,
    zs,
    zr,
    own,
    part,
    ps,
    pr,
    red,
    fwd_in,
    top_in,
    low_in,
    low_out,
    fin,
    zback,
    zret,
    st_s,
    st_r,
    local_sem,
    send_sem,
    recv_sem,
):
    ep = lax.axis_index("ep")
    core = lax.axis_index("tp")
    x = lax.rem(ep, NX)
    y = lax.rem(ep // NX, NY)
    z = ep // (NX * NY)

    def device(dx=0, dy=0, dz=0, flip=False):
        ex = lax.rem(x + (dx + NX), NX)
        ey = lax.rem(y + (dy + NY), NY)
        ez = lax.rem(z + (dz + NZ), NZ)
        return {"ep": (ez * NY + ey) * NX + ex, "tp": (1 - core) if flip else core}

    def along(first, step):
        return device(dx=step) if first else device(dy=step)

    pair = device(flip=True)
    peers = [pair]
    peers += [device(dz=d) for d in OFFZ[1:]]
    peers += [device(dx=d) for d in OFF[1:]]
    peers += [device(dy=d) for d in OFF[1:]]
    barrier = pltpu.get_barrier_semaphore()
    for peer in peers:
        pl.semaphore_signal(barrier, inc=1, device_id=peer, device_id_type=MESH)

    loads = []
    for n, (src, dst) in enumerate(
        (
            (wo_hbm, wo_v),
            (router_hbm, router_v),
            (gate_hbm.at[0], gate_v),
            (up_hbm.at[0], up_v),
            (down_hbm.at[0], down_v),
        )
    ):
        load = pltpu.make_async_copy(src, dst, local_sem.at[n])
        load.start()
        loads.append(load)

    made = []

    def send(src, dst, to):
        n = len(made)
        copy = pltpu.make_async_remote_copy(
            src_ref=src,
            dst_ref=dst,
            send_sem=send_sem.at[n],
            recv_sem=recv_sem.at[n],
            device_id=to,
            device_id_type=MESH,
        )
        copy.start()
        made.append(copy)
        return copy

    loads[0].wait()
    partial_bf = dotf(gated_ref[...], wo_v[...]).astype(BF16)
    xs[...] = partial_bf
    pl.semaphore_wait(barrier, len(peers))
    exchange = send(xs, xr, pair)
    mixed = ROOT2 * tokens_ref[...].astype(F32) + partial_bf.astype(F32)

    routes = routes_ref[...]
    first_route, second_route = routes[:, 0:1], routes[:, 1:2]
    group_col = lax.shift_right_logical(first_route, 6)
    lanes = iota((ROWS, 128), 1)
    onehot_group = where_bf16(lanes == group_col)
    lower = where_bf16(iota((ROWS, ROWS), 0) > iota((ROWS, ROWS), 1))
    earlier = dotf(lower, onehot_group)
    rank_col = jnp.sum(jnp.where(lanes == group_col, earlier, 0.0), axis=1, keepdims=True)
    place_col = group_col.astype(F32) * 4.0 + rank_col
    diagonal = jnp.where(iota((ROWS, ROWS), 0) == iota((ROWS, ROWS), 1), place_col, 0.0)
    place_row = dotf(jnp.ones((64, ROWS), BF16), diagonal.astype(BF16))
    slab_row = iota((64, ROWS), 0)
    wanted = ((slab_row >> 4) * 4 + (slab_row & 3)).astype(F32)
    quarter = (slab_row >> 2) & 3
    match = place_row == wanted

    exchange.wait_recv()
    mixed = mixed + xr[...].astype(F32)
    mean = jnp.mean(mixed, axis=-1, keepdims=True)
    centered = mixed - mean
    spread = jnp.mean(centered * centered, axis=-1, keepdims=True)
    hidden = (
        centered * lax.rsqrt(spread + EPS) * gain_ref[0:1, :] + bias_ref[0:1, :]
    ).astype(BF16)
    hid[...] = hidden

    loads[1].wait()
    expert_logit = dotf(hidden, router_v[...])
    hidden_f = hidden.astype(F32)
    group_logit = [
        jnp.sum(hidden_f * group_ref[g : g + 1, :].astype(F32), axis=1, keepdims=True)
        for g in range(4)
    ]
    own_logit = jnp.zeros_like(group_logit[0])
    for g in range(4):
        own_logit = own_logit + jnp.where(group_col == g, group_logit[g], 0.0)
    share_sum = jnp.zeros_like(own_logit)
    for g in range(4):
        share_sum = share_sum + jnp.exp(group_logit[g] - own_logit)
    share = 1.0 / share_sum
    wide = iota((ROWS, 256), 1)
    picked0 = jnp.sum(jnp.where(wide == first_route, expert_logit, 0.0), axis=1, keepdims=True)
    picked1 = jnp.sum(jnp.where(wide == second_route, expert_logit, 0.0), axis=1, keepdims=True)
    weight0 = share * jax.nn.sigmoid(picked0 - picked1)
    weight1 = share * jax.nn.sigmoid(picked1 - picked0)
    meta = (
        jnp.where(lanes == (first_route & 63), weight0, 0.0)
        + jnp.where(lanes == (second_route & 63), weight1, 0.0)
    ).astype(BF16)

    my_cols = pl.multiple_of(core * HALF, HALF)
    other_cols = pl.multiple_of((1 - core) * HALF, HALF)
    slabs = jnp.zeros((64, FOLD), F32)
    for q in range(4):
        pick = where_bf16(match & (quarter == q))
        slabs = slabs + dotf(pick, hid[:, pl.ds(pl.multiple_of(my_cols + q * FOLD, FOLD), FOLD)])
    slab_meta = dotf(where_bf16(match & (quarter == 0)), meta)
    zs[:, :, 0:FOLD] = slabs.astype(BF16).reshape(4, 16, FOLD)
    zs[:, :, FOLD:SLAB] = slab_meta.astype(BF16).reshape(4, 16, 128)
    z_sends = [None]
    for k in range(1, NZ):
        to_z = lax.rem(z + (OFFZ[k] + NZ), NZ)
        z_sends.append(send(zs.at[to_z // 2], zr.at[k], device(dz=OFFZ[k])))
    zr[0] = zs[z // 2]

    out_i = iota((64, 64), 0)
    in_i = iota((64, 64), 1)
    unfold = where_bf16(
        in_i == ((out_i >> 2) & 3) * 16 + (out_i >> 4) * 4 + (out_i & 3)
    )

    def slot(i, h, j):
        return i * 8 + h * 4 + j

    arrive = {}

    def p1_sends(h):
        for j in (3, 1, 2):
            arrive[0, h, j] = send(
                own.at[slot(0, h, 0)], own.at[slot(0, h, j)], along(h == 0, OFF[j])
            )

    def p2_sends(h, j):
        for i in (1, 2):
            arrive[i, h, j] = send(
                own.at[slot(0, h, j)], own.at[slot(i, h, j)], along(h == 1, OFF[i])
            )

    def forward(h, j):
        i = 1 if j in VIA_PLUS else 2
        arrive[i, h, j].wait_recv()
        arrive[3, h, j] = send(
            own.at[slot(i, h, j)], own.at[slot(3, h, j)], along(h == 1, OFF[i])
        )

    def to_pair(first, count):
        return send(
            own.at[pl.ds(first, count), :, pl.ds(0, HALF)],
            part.at[pl.ds(first, count)],
            pair,
        )

    for h in range(2):
        for k in range(4 * h, 4 * h + 4):
            if k:
                z_sends[k].wait_recv()
        block = dotf(unfold, zr[4 * h : 4 * h + 4].reshape(64, SLAB)).astype(BF16)
        for q in range(4):
            own[slot(0, h, 0), :, q * FOLD : (q + 1) * FOLD] = block[
                q * 16 : (q + 1) * 16, 0:FOLD
            ]
        own[slot(0, h, 0), :, HALF:CARRY] = block[0:16, FOLD:SLAB]
        p1_sends(h)
        p2_sends(h, 0)

    half_copies = {}
    for h in range(2):
        for j in (1, 2, 3):
            arrive[0, h, j].wait_recv()
            p2_sends(h, j)
        half_copies[0, h] = to_pair(slot(0, h, 0), 4)
    my_expert = lax.rem(ep, 32) * 2 + core

    def experts(i, count):
        rows = count * 128
        first = i * 8
        mine = own[first : first + count * 8, :, 0:HALF].reshape(rows, HALF)
        theirs = part[first : first + count * 8].reshape(rows, HALF)
        marks = own[first : first + count * 8, :, HALF:CARRY].reshape(rows, 128).astype(F32)
        weight = jnp.sum(
            jnp.where(iota((rows, 128), 1) == my_expert, marks, 0.0), axis=1, keepdims=True
        )
        my_rows, other_rows = pl.ds(my_cols, HALF), pl.ds(other_cols, HALF)
        gate = dotf(mine, gate_v[my_rows, :]) + dotf(theirs, gate_v[other_rows, :])
        up = dotf(mine, up_v[my_rows, :]) + dotf(theirs, up_v[other_rows, :])
        act = (jax.nn.silu(gate) * up).astype(BF16)
        away = dotf(act, down_v[:, pl.ds(other_cols, HALF)]) * weight
        ps[first : first + count * 8] = away.astype(BF16).reshape(count * 8, 16, HALF)
        copy = send(
            ps.at[pl.ds(first, count * 8)], pr.at[pl.ds(first, count * 8)], pair
        )
        here = dotf(act, down_v[:, pl.ds(my_cols, HALF)]) * weight
        red[first : first + count * 8] = here.astype(BF16).reshape(count * 8, 16, HALF)
        return copy

    def add_pair(copy, i, count):
        copy.wait_recv()
        span = slice(i * 8, (i + count) * 8)
        red[span] = (red[span].astype(F32) + pr[span].astype(F32)).astype(BF16)

    for load in loads[2:]:
        load.wait()
    for h in range(2):
        half_copies[0, h].wait_recv()
    result0 = experts(0, 1)
    for j in (0, 1, 2, 3):
        for h in range(2):
            forward(h, j)
    for i in (1, 2):
        for h in range(2):
            for j in range(4):
                if (i == 1) != (j in VIA_PLUS):
                    arrive[i, h, j].wait_recv()
    middle = to_pair(8, 16)
    add_pair(result0, 0, 1)
    middle.wait_recv()
    result1 = experts(1, 2)
    for h in range(2):
        for j in range(4):
            arrive[3, h, j].wait_recv()
    last = to_pair(24, 8)
    add_pair(result1, 1, 2)

    top = {}

    def top_send(i, h, j):
        top[i, h, j] = send(
            red.at[slot(i, h, j)],
            top_in.at[(i - 1) * 8 + h * 4 + j],
            along(h == 1, -OFF[i]),
        )

    for h in range(2):
        for j in VIA_MINUS:
            top_send(1, h, j)
        for j in VIA_PLUS:
            top_send(2, h, j)
    last.wait_recv()
    result2 = experts(3, 1)
    add_pair(result2, 3, 1)
    back = {}
    for h in range(2):
        for j in range(4):
            i = 1 if j in VIA_PLUS else 2
            back[h, j] = send(
                red.at[slot(3, h, j)], fwd_in.at[h * 4 + j], along(h == 1, -OFF[i])
            )
    for h in range(2):
        for j in range(4):
            i = 1 if j in VIA_PLUS else 2
            back[h, j].wait_recv()
            s = slot(i, h, j)
            red[s] = (red[s].astype(F32) + fwd_in[h * 4 + j].astype(F32)).astype(BF16)
            top_send(i, h, j)
    low = {}
    for j in (3, 1, 2, 0):
        for h in range(2):
            total = red[slot(0, h, j)].astype(F32)
            for i in (1, 2):
                top[i, h, j].wait_recv()
                total = total + top_in[(i - 1) * 8 + h * 4 + j].astype(F32)
            if j:
                low_out[h * 4 + j] = total.astype(BF16)
                low[h, j] = send(
                    low_out.at[h * 4 + j], low_in.at[h * 4 + j], along(h == 0, -OFF[j])
                )
            else:
                fin[h] = total

    fold_i = iota((64, 16), 0)
    fold_o = iota((64, 16), 1)
    fold_match = fold_o == (fold_i >> 4) * 4 + (fold_i & 3)
    fold_quarter = (fold_i >> 2) & 3
    z_back = [None]
    for h in range(2):
        total = fin[h]
        for j in (1, 2, 3):
            low[h, j].wait_recv()
            total = total + low_in[h * 4 + j].astype(F32)
        total = total.astype(BF16)
        folded = jnp.zeros((64, FOLD), F32)
        for q in range(4):
            folded = folded + dotf(
                where_bf16(fold_match & (fold_quarter == q)),
                total[:, q * FOLD : (q + 1) * FOLD],
            )
        zback[4 * h : 4 * h + 4] = folded.astype(BF16).reshape(4, 16, FOLD)
        for k in range(4 * h, 4 * h + 4):
            if k:
                z_back.append(send(zback.at[k], zret.at[k], device(dz=-OFFZ[k])))
    zret[0] = zback[0]

    take_o = iota((64, 128), 0)
    take_i = iota((64, 128), 1)
    slab_k = take_i >> 4
    away_k = (slab_k + 1) >> 1
    signed = jnp.where((slab_k & 1) == 1, away_k, -away_k)
    plane = (z + signed + NZ) & (NZ - 1)
    expected = ((plane >> 1) * 4 + (take_i & 3)).astype(F32)
    place_tall = jnp.concatenate([place_col] * 4, axis=0)
    take = where_bf16(
        (expected == place_tall) & ((take_o >> 4) == ((take_i >> 2) & 3))
    )
    for k in range(1, NZ):
        z_back[k].wait_recv()
    routed = dotf(take, zret[...].reshape(128, FOLD))
    routed = jnp.concatenate([routed[q * 16 : (q + 1) * 16] for q in range(4)], axis=1)
    blended = ROOT2 * hid[:, pl.ds(my_cols, HALF)].astype(F32) + routed
    row_sum = jnp.sum(blended, axis=1, keepdims=True)
    row_sq = jnp.sum(blended * blended, axis=1, keepdims=True)
    st_s[...] = jnp.where(lanes == 0, row_sum, row_sq)
    stats = send(st_s, st_r, pair)
    stats.wait_recv()
    row_mean = (row_sum + st_r[:, 0:1]) / WIDTH
    spread = (row_sq + st_r[:, 1:2]) / WIDTH - row_mean * row_mean
    out_ref[...] = (
        (blended - row_mean)
        * lax.rsqrt(spread + EPS)
        * gain_ref[1:2, pl.ds(my_cols, HALF)]
        + bias_ref[1:2, pl.ds(my_cols, HALF)]
    ).astype(BF16)
    for copy in made:
        copy.wait_send()


def moe(gated, tokens, gain, bias, group_rows, routes, wo, router, gate, up, down):
    vmem = pl.BlockSpec(memory_space=pltpu.VMEM)
    anywhere = pl.BlockSpec(memory_space=pl.ANY)
    return pl.pallas_call(
        moe_kernel,
        out_shape=jax.ShapeDtypeStruct((ROWS, HALF), BF16),
        in_specs=[vmem] * 6 + [anywhere] * 5,
        out_specs=vmem,
        scratch_shapes=[
            pltpu.VMEM((512, WIDTH), BF16),
            pltpu.VMEM((WIDTH, 256), BF16),
            pltpu.VMEM((WIDTH, 256), BF16),
            pltpu.VMEM((WIDTH, 256), BF16),
            pltpu.VMEM((256, WIDTH), BF16),
            pltpu.VMEM((ROWS, WIDTH), BF16),
            pltpu.VMEM((ROWS, WIDTH), BF16),
            pltpu.VMEM((ROWS, WIDTH), BF16),
            pltpu.VMEM((4, 16, SLAB), BF16),
            pltpu.VMEM((8, 16, SLAB), BF16),
            pltpu.VMEM((32, 16, CARRY), BF16),
            pltpu.VMEM((32, 16, HALF), BF16),
            pltpu.VMEM((32, 16, HALF), BF16),
            pltpu.VMEM((32, 16, HALF), BF16),
            pltpu.VMEM((32, 16, HALF), BF16),
            pltpu.VMEM((8, 16, HALF), BF16),
            pltpu.VMEM((16, 16, HALF), BF16),
            pltpu.VMEM((8, 16, HALF), BF16),
            pltpu.VMEM((8, 16, HALF), BF16),
            pltpu.VMEM((2, 16, HALF), F32),
            pltpu.VMEM((8, 16, FOLD), BF16),
            pltpu.VMEM((8, 16, FOLD), BF16),
            pltpu.VMEM((ROWS, 128), F32),
            pltpu.VMEM((ROWS, 128), F32),
            pltpu.SemaphoreType.DMA((5,)),
            pltpu.SemaphoreType.DMA((NCOPY,)),
            pltpu.SemaphoreType.DMA((NCOPY,)),
        ],
        compiler_params=pltpu.CompilerParams(
            collective_id=0, has_side_effects=True, vmem_limit_bytes=60 * 1024 * 1024
        ),
        name="route_and_experts",
    )(gated, tokens, gain, bias, group_rows, routes, wo, router, gate, up, down)


CHUNK = 2
NCHUNK = ROWS // CHUNK


def attention_kernel(
    tokens_ref,
    head_gain_ref,
    key_hbm,
    value_hbm,
    decay_hbm,
    query_hbm,
    gate_hbm,
    state_hbm,
    gated_ref,
    new_hbm,
    key_v,
    value_v,
    decay_v,
    query_v,
    gate_v,
    state_v,
    columns,
    values,
    readout,
    load_sem,
    in_sem,
    out_sem,
):
    loads = []
    for n, (src, dst) in enumerate(
        (
            (decay_hbm, decay_v),
            (key_hbm, key_v),
            (query_hbm, query_v),
            (value_hbm, value_v),
        )
    ):
        load = pltpu.make_async_copy(src, dst, load_sem.at[n])
        load.start()
        loads.append(load)
    states = []
    for n in range(NCHUNK):
        span = pl.ds(n * CHUNK, CHUNK)
        load = pltpu.make_async_copy(state_hbm.at[span], state_v.at[span], in_sem.at[n])
        load.start()
        states.append(load)
    gate_load = pltpu.make_async_copy(gate_hbm, gate_v, load_sem.at[4])
    gate_load.start()

    tokens = tokens_ref[...]
    loads[0].wait()
    decay = jnp.exp(jax.nn.log_sigmoid(dotf(tokens, decay_v[...])) / 16.0)
    loads[1].wait()
    keys = dotf(tokens, key_v[...])
    loads[2].wait()
    queries = dotf(tokens, query_v[...]) * 128 ** (-0.5)
    stacked = jnp.concatenate(
        [decay, keys, queries, jnp.zeros((128 - 3 * ROWS, 256), F32)], axis=0
    )
    columns[...] = stacked.T
    loads[3].wait()
    values[...] = dotf(tokens, value_v[...])

    stores = []
    for n in range(NCHUNK):
        states[n].wait()
        for b in range(n * CHUNK, (n + 1) * CHUNK):
            for h in range(2):
                rows = slice(h * 128, (h + 1) * 128)
                decay_col = columns[rows, b : b + 1]
                key_col = columns[rows, ROWS + b : ROWS + b + 1]
                query_col = columns[rows, 2 * ROWS + b : 2 * ROWS + b + 1]
                value_row = values[b : b + 1, h * 256 : (h + 1) * 256]
                fresh = decay_col * state_v[b, h] + key_col * value_row
                state_v[b, h] = fresh
                readout[b : b + 1, h * 256 : (h + 1) * 256] = jnp.sum(
                    query_col * fresh, axis=0, keepdims=True
                )
        span = pl.ds(n * CHUNK, CHUNK)
        store = pltpu.make_async_copy(state_v.at[span], new_hbm.at[span], out_sem.at[n])
        store.start()
        stores.append(store)

    gate_load.wait()
    gate_rows = dotf(tokens, gate_v[...])
    for h in range(2):
        cols = slice(h * 256, (h + 1) * 256)
        read = readout[:, cols]
        scale = lax.rsqrt(jnp.mean(read * read, axis=-1, keepdims=True) + EPS)
        gated_ref[:, cols] = (
            read * scale * head_gain_ref[...] * jax.nn.silu(gate_rows[:, cols])
        ).astype(BF16)
    for store in stores:
        store.wait()


def attention(tokens, head_gain, key_w, value_w, decay_w, query_w, gate_w, state):
    vmem = pl.BlockSpec(memory_space=pltpu.VMEM)
    anywhere = pl.BlockSpec(memory_space=pl.ANY)
    return pl.pallas_call(
        attention_kernel,
        out_shape=(
            jax.ShapeDtypeStruct((ROWS, 512), BF16),
            jax.ShapeDtypeStruct(state.shape, F32),
        ),
        in_specs=[vmem] * 2 + [anywhere] * 6,
        out_specs=(vmem, anywhere),
        scratch_shapes=[
            pltpu.VMEM((WIDTH, 256), BF16),
            pltpu.VMEM((WIDTH, 512), BF16),
            pltpu.VMEM((WIDTH, 256), BF16),
            pltpu.VMEM((WIDTH, 256), BF16),
            pltpu.VMEM((WIDTH, 512), BF16),
            pltpu.VMEM((ROWS, 2, 128, 256), F32),
            pltpu.VMEM((256, 128), F32),
            pltpu.VMEM((ROWS, 512), F32),
            pltpu.VMEM((ROWS, 512), F32),
            pltpu.SemaphoreType.DMA((5,)),
            pltpu.SemaphoreType.DMA((NCHUNK,)),
            pltpu.SemaphoreType.DMA((NCHUNK,)),
        ],
        compiler_params=pltpu.CompilerParams(vmem_limit_bytes=60 * 1024 * 1024),
        cost_estimate=pl.CostEstimate(
            flops=150_000_000, bytes_accessed=15_000_000, transcendentals=10_000
        ),
        name="attention_state",
    )(tokens, head_gain, key_w, value_w, decay_w, query_w, gate_w, state)


def on_device(
    tokens,
    recurrent_state,
    query_weight,
    key_weight,
    decay_weight,
    value_weight,
    gate_weight,
    head_gain,
    output_weight,
    norm_gain,
    norm_bias,
    group_router,
    router_weight,
    routes,
    expert_gate,
    expert_up,
    expert_down,
):
    gated_rows, new_state = attention(
        tokens,
        head_gain.reshape(1, 256),
        key_weight,
        value_weight,
        decay_weight,
        query_weight,
        gate_weight,
        recurrent_state,
    )
    new_tokens = moe(
        gated_rows,
        tokens,
        norm_gain,
        norm_bias,
        group_router.T,
        routes,
        output_weight,
        router_weight,
        expert_gate,
        expert_up,
        expert_down,
    )
    return (new_tokens, new_state)


def solution(mesh):
    in_specs = (
        P("ep", None),
        P("ep", "tp", None, None),
        P(None, "tp"),
        P(None, "tp"),
        P(None, "tp"),
        P(None, "tp"),
        P(None, "tp"),
        P(),
        P("tp", None),
        P(),
        P(),
        P(),
        P(),
        P("ep", None),
        P(("ep", "tp"), None, None),
        P(("ep", "tp"), None, None),
        P(("ep", "tp"), None, None),
    )
    out_specs = (P("ep", "tp"), P("ep", "tp", None, None))
    return jax.shard_map(
        on_device, mesh=mesh, in_specs=in_specs, out_specs=out_specs, check_vma=False
    )
```
